256 devices in a mesh: fs: 32 (over z, y), tp: 8 (over x, core).
Axes of the slice: x: 4, y: 4, z: 8, core: 2. Of those that a mesh axis runs over, the one named last changes fastest.
Arguments:
- latent_in: bfloat16 [98304, 512], P('fs'), may hold values from -6 to 6
- query_cot: bfloat16 [98304, 1536], P('fs', 'tp'), may hold values from -6 to 6
- attn_out: bfloat16 [98304, 1024], P('fs'), may hold values from -6 to 6
- mix_cot: bfloat16 [98304, 2048], P('fs', 'tp'), may hold values from -6 to 6
- query_weight: float32 [512, 1536], P('fs', 'tp'), may hold values from -0.25 to 0.25
- output_weight: float32 [1024, 2048], P('fs', 'tp'), may hold values from -0.1875 to 0.1875
- query_factor: bfloat16 [512, 256], P('fs'), may hold values from -0.25 to 0.25
- output_factor: bfloat16 [1024, 256], P('fs'), may hold values from -0.1875 to 0.1875
- query_mean: float32 [256, 1536], P('fs', 'tp'), may hold values from -3 to 3
- query_square: float32 [256, 1536], P('fs', 'tp'), may hold values from 0.05 to 1
- output_mean: float32 [256, 2048], P('fs', 'tp'), may hold values from -3 to 3
- output_square: float32 [256, 2048], P('fs', 'tp'), may hold values from 0.05 to 1
Outputs:
- step_query: float32 [512, 1536], P('fs', 'tp')
- step_output: float32 [1024, 2048], P('fs', 'tp')
- new_query: float32 [512, 1536], P('fs', 'tp')
- new_output: float32 [1024, 2048], P('fs', 'tp')
- copy_query: bfloat16 [512, 1536], P(None, 'tp')
- copy_output: bfloat16 [1024, 2048], P(None, 'tp')
- query_mean_new: float32 [256, 1536], P('fs', 'tp')
- query_square_new: float32 [256, 1536], P('fs', 'tp')
- output_mean_new: float32 [256, 2048], P('fs', 'tp')
- output_square_new: float32 [256, 2048], P('fs', 'tp')
The draws below stay inside these ranges and needn't reach their ends.
All inputs are finite; a program needn't handle non-finite values.
Results may differ from the reference program's by a relative error of at most 0.0085.
Values may be sent and summed in bfloat16 or wider, within the bound.
No kernel may reach another device: no remote copies, remote signals or barrier semaphores. Data moves between devices by JAX's collectives and lax.ppermute only.
A program may use at most 64 MiB of HBM per device.

```python
import math
import jax
import jax.numpy as jnp
from jax import lax

D = 2048
Q_RANK = 512
RANK = 256
QCOLS = 1536
HV = 1024
TOKENS = 98304


def level_of(key, extent, cuts, smallest, top_value):
    loudness, own = 1.0, jax.random.fold_in(key, 6)
    for axis_at, blocks in cuts:
        draws = jnp.exp(jax.random.uniform(jax.random.fold_in(own, axis_at), (blocks,), jnp.float32, smallest / len(cuts), top_value / len(cuts)))
        loudness = loudness * jnp.repeat(draws, extent[axis_at] // blocks).reshape([-1 if axis == axis_at else 1 for axis in range(len(extent))])
    return loudness


def normal_values(rng, extent, width, limit, shards=(), held_as=jnp.bfloat16):
    factor_of = level_of(rng, extent, shards, -0.22, 0.18) if shards else 1.0
    values = jax.random.normal(rng, extent, jnp.float32) * width * factor_of
    return jnp.minimum(jnp.maximum(values, -limit), limit).astype(held_as)


def setup_inputs(seed: int = 0) -> dict:
    key_of = jax.random.split(jax.random.key(seed), 13)
    latent_in = normal_values(key_of[0], (TOKENS, Q_RANK), 1.0, 6.0, ((0, 32),))
    query_cot = normal_values(key_of[1], (TOKENS, QCOLS), 1.0, 6.0, ((0, 32), (1, 8)))
    attn_out = normal_values(key_of[2], (TOKENS, HV), 1.0, 6.0, ((0, 32),))
    mix_cot = normal_values(key_of[3], (TOKENS, D), 1.0, 6.0, ((0, 32), (1, 8)))
    query_weight = normal_values(key_of[4], (Q_RANK, QCOLS), Q_RANK ** -0.5, 0.25, ((0, 32), (1, 8)), jnp.float32)
    output_weight = normal_values(key_of[5], (HV, D), HV ** -0.5, 0.1875, ((0, 32), (1, 8)), jnp.float32)
    query_factor = normal_values(key_of[6], (Q_RANK, RANK), Q_RANK ** -0.5, 0.25, ((0, 32),))
    output_factor = normal_values(key_of[7], (HV, RANK), HV ** -0.5, 0.1875, ((0, 32),))
    query_mean = normal_values(key_of[8], (RANK, QCOLS), 0.5, 3.0, ((0, 32), (1, 8)), jnp.float32)
    query_square = jnp.clip(jnp.exp(math.log(1.0) - 2.9957323 * jax.random.uniform(key_of[9], (RANK, QCOLS), jnp.float32) ** level_of(key_of[9], (RANK, QCOLS), ((0, 32), (1, 8)), -0.2, 0.2)), 0.05, 1.0)
    output_mean = normal_values(key_of[10], (RANK, D), 0.5, 3.0, ((0, 32), (1, 8)), jnp.float32)
    output_square = jnp.clip(jnp.exp(math.log(1.0) - 2.9957323 * jax.random.uniform(key_of[11], (RANK, D), jnp.float32) ** level_of(key_of[11], (RANK, D), ((0, 32), (1, 8)), -0.2, 0.2)), 0.05, 1.0)
    return {"latent_in": latent_in, "query_cot": query_cot, "attn_out": attn_out, "mix_cot": mix_cot, "query_weight": query_weight, "output_weight": output_weight, "query_factor": query_factor, "output_factor": output_factor, "query_mean": query_mean, "query_square": query_square, "output_mean": output_mean, "output_square": output_square}


def over_rows(left, right):
    return lax.dot_general(left, right, (((0,), (0,)), ((), ())), preferred_element_type=jnp.float32)

def exact_dot(left, right):
    return jnp.dot(left, right, precision=lax.Precision.HIGHEST, preferred_element_type=jnp.float32)

def moments(mean, square, low):
    mean_new = 0.8 * mean + 0.2 * low
    square_new = 0.9 * square + 0.1 * low * low
    return (mean_new, square_new, mean_new / jnp.sqrt(square_new))

def reference(latent_in, query_cot, attn_out, mix_cot, query_weight, output_weight, query_factor, output_factor, query_mean, query_square, output_mean, output_square):
    inv_root = 1.0 / math.sqrt(latent_in.shape[0])
    grad_query = over_rows(latent_in, query_cot) * inv_root
    grad_output = over_rows(attn_out, mix_cot) * inv_root
    factor_query = query_factor.astype(jnp.float32)
    factor_output = output_factor.astype(jnp.float32)
    low_query = exact_dot(factor_query.T, grad_query)
    low_output = exact_dot(factor_output.T, grad_output)
    mean_q, square_q, direction_q = moments(query_mean, query_square, low_query)
    mean_o, square_o, direction_o = moments(output_mean, output_square, low_output)
    scale_q = 1.0 / jnp.sqrt(jnp.mean(direction_q * direction_q) + 0.25)
    scale_o = 1.0 / jnp.sqrt(jnp.mean(direction_o * direction_o) + 0.25)
    step_q = exact_dot(factor_query, direction_q) * scale_q
    step_o = exact_dot(factor_output, direction_o) * scale_o
    new_q = query_weight - 0.02 * step_q
    new_o = output_weight - 0.02 * step_o
    return (step_q, step_o, new_q, new_o, new_q.astype(jnp.bfloat16), new_o.astype(jnp.bfloat16), mean_q, square_q, mean_o, square_o)
```

```python
import math

import jax
import jax.numpy as jnp
from jax import lax
from jax.sharding import PartitionSpec as P


def exchange(tiles, axis):
    return lax.all_to_all(tiles, axis, split_axis=0, concat_axis=0, tiled=True)


def sent_to_all(x, axis):
    return exchange(jnp.broadcast_to(x, (lax.axis_size(axis), *x.shape)), axis)


def contract(left, right, dims):
    return lax.dot_general(left, right, (dims, ((), ())), preferred_element_type=jnp.float32)


def moments(mean, square, low):
    mean_new = 0.8 * mean + 0.2 * low
    square_new = 0.9 * square + 0.1 * low * low
    return (mean_new, square_new, mean_new / jnp.sqrt(square_new))


def on_device(
    latent_in,
    query_cot,
    attn_out,
    mix_cot,
    query_weight,
    output_weight,
    query_factor,
    output_factor,
    query_mean,
    query_square,
    output_mean,
    output_square,
):
    bf16 = jnp.bfloat16
    count = lax.axis_size("fs")
    columns = lax.axis_size("tp")
    inv_root = 1.0 / math.sqrt(latent_in.shape[0] * count)
    rows_q, width_q = query_weight.shape
    rows_o, width_o = output_weight.shape
    rank = query_factor.shape[1]

    factors = sent_to_all(jnp.concatenate([query_factor, output_factor], axis=0), "fs")
    padded = jnp.pad(query_weight.astype(bf16), ((0, 0), (0, width_o - width_q)))
    weights = sent_to_all(jnp.concatenate([padded, output_weight.astype(bf16)], axis=0), "fs")

    grad_q = contract(latent_in, query_cot, ((0,), (0,))).astype(bf16)
    grad_o = contract(attn_out, mix_cot, ((0,), (0,))).astype(bf16)
    factor_q = factors[:, :rows_q].reshape(count * rows_q, rank)
    factor_o = factors[:, rows_q:].reshape(count * rows_o, rank)
    low = jnp.concatenate(
        [contract(factor_q, grad_q, ((0,), (0,))), contract(factor_o, grad_o, ((0,), (0,)))], axis=1
    )
    low = (low * inv_root).astype(bf16).reshape(count, rank // count, width_q + width_o)
    low = jnp.sum(exchange(low, "fs").astype(jnp.float32), axis=0)

    mean_q, square_q, direction_q = moments(query_mean, query_square, low[:, :width_q])
    mean_o, square_o, direction_o = moments(output_mean, output_square, low[:, width_q:])
    joined = jnp.concatenate([direction_q, direction_o], axis=1).astype(bf16)
    piece = sent_to_all(joined, "fs").reshape(rank, width_q + width_o)
    piece_q, piece_o = piece[:, :width_q], piece[:, width_q:]

    squares = jnp.sum(jnp.square(piece.astype(jnp.float32)), axis=0)
    sums = jnp.stack([jnp.sum(squares[:width_q]), jnp.sum(squares[width_q:])])
    sums = jnp.sum(sent_to_all(sums.reshape(1, 2), "tp"), axis=0)[0]
    scale_q = 1.0 / jnp.sqrt(sums[0] / (rank * width_q * columns) + 0.25)
    scale_o = 1.0 / jnp.sqrt(sums[1] / (rank * width_o * columns) + 0.25)

    step_q = contract(query_factor, piece_q, ((1,), (0,))) * scale_q
    step_o = contract(output_factor, piece_o, ((1,), (0,))) * scale_o
    new_q = query_weight - 0.02 * step_q
    new_o = output_weight - 0.02 * step_o

    whole_q = weights[:, :rows_q, :width_q].reshape(count * rows_q, width_q)
    whole_o = weights[:, rows_q:].reshape(count * rows_o, width_o)
    step_all_q = contract(factor_q, piece_q, ((1,), (0,))) * scale_q
    step_all_o = contract(factor_o, piece_o, ((1,), (0,))) * scale_o
    copy_q = (whole_q.astype(jnp.float32) - 0.02 * step_all_q).astype(bf16)
    copy_o = (whole_o.astype(jnp.float32) - 0.02 * step_all_o).astype(bf16)
    return (step_q, step_o, new_q, new_o, copy_q, copy_o, mean_q, square_q, mean_o, square_o)


def solution(mesh):
    rows = P("fs", None)
    both = P("fs", "tp")
    gathered = P(None, "tp")
    return jax.shard_map(
        on_device,
        mesh=mesh,
        in_specs=(rows, both, rows, both, both, both, rows, rows, both, both, both, both),
        out_specs=(both, both, both, both, gathered, gathered, both, both, both, both),
        check_vma=False,
    )
```

```python
import functools
import math

import jax
import jax.numpy as jnp
from jax import lax
from jax.experimental import pallas as pl
from jax.experimental.pallas import tpu as pltpu
from jax.sharding import PartitionSpec as P

BF16 = jnp.bfloat16
F32 = jnp.float32
LANES = 128
RING = 4


def exchange(tiles, axis):
    return lax.all_to_all(tiles, axis, split_axis=0, concat_axis=0, tiled=True)


def contract(left, right, left_dim, right_dim):
    dims = (((left_dim,), (right_dim,)), ((), ()))
    return lax.dot_general(left, right, dims, preferred_element_type=F32)


def on_chip(body, outs, *args, scratch=()):
    vmem = pl.BlockSpec(memory_space=pltpu.VMEM)
    return pl.pallas_call(
        body,
        out_shape=tuple(jax.ShapeDtypeStruct(s, d) for s, d in outs),
        in_specs=[vmem] * len(args),
        out_specs=tuple(vmem for _ in outs),
        scratch_shapes=list(scratch),
    )(*args)


def halves(x):
    return x[:, :LANES], x[:, LANES:]


def pack_body(fq, fo, wq, wo, out):
    count = out.shape[0]
    core = lax.axis_index("tp") % 2
    rows_q, rows_o = fq.shape[0], fo.shape[0]
    rows = rows_q + rows_o
    for f, at in ((fq, 0), (fo, rows_q)):
        left, right = halves(f[...])
        half = jnp.where(core == 0, left.astype(F32), right.astype(F32)).astype(BF16)
        out[:, at : at + f.shape[0]] = jnp.broadcast_to(half, (count, *half.shape))
    width_q = wq.shape[1]
    for y in range(RING):
        row, col = y % 2, y // 2
        part = wq[8 * row : 8 * row + 8, col * LANES : min(width_q, (col + 1) * LANES)]
        if part.shape[1] < LANES:
            part = jnp.concatenate([part, jnp.zeros((8, LANES - part.shape[1]), F32)], axis=1)
        left, right = halves(wo[8 * y : 8 * y + 8, :])
        quarter = jnp.concatenate([part, left, right], axis=0).astype(BF16)
        for z in range(count // RING):
            out[z * RING + y, rows:] = quarter


def low_body(inv_root, rows_q, rows, own, other, gq_t, go, out):
    count = own.shape[0]
    core = lax.axis_index("tp") % 2
    width_q = gq_t.shape[0]
    part = (count // 2, LANES * 2 // count, -1)
    for ref, at in ((own, core), (other, 1 - core)):
        fq = ref[:, :rows_q].reshape(count * rows_q, LANES)
        fo = ref[:, rows_q:rows].reshape(count * (rows - rows_q), LANES)
        low_q = contract(gq_t[...], fq, 1, 0).T * inv_root
        low_o = contract(fo, go[...], 0, 0) * inv_root
        to = pl.ds(at * (count // 2), count // 2)
        out[to, :, :width_q] = low_q.reshape(part).astype(BF16)
        out[to, :, width_q:] = low_o.reshape(part).astype(BF16)


def moments_body(parts, mq, sq, mo, so, mq_new, sq_new, mo_new, so_new, out):
    low = jnp.sum(parts[...].astype(F32), axis=0)
    width_q = mq.shape[1]
    count = out.shape[0]
    for piece, mean, square, mean_out, square_out, at in (
        (low[:, :width_q], mq, sq, mq_new, sq_new, slice(0, width_q)),
        (low[:, width_q:], mo, so, mo_new, so_new, slice(width_q, None)),
    ):
        mean_new = 0.8 * mean[...] + 0.2 * piece
        square_new = 0.9 * square[...] + 0.1 * piece * piece
        mean_out[...] = mean_new
        square_out[...] = square_new
        direction = (mean_new / jnp.sqrt(square_new)).astype(BF16)
        out[:, :, at] = jnp.broadcast_to(direction, (count, *direction.shape))


def sums_body(width_q, piece, out):
    x = piece[...].astype(F32)
    squares = jnp.sum(jnp.sum(x * x, axis=0), axis=0, keepdims=True)
    half = (out.shape[0], out.shape[1] // 2, out.shape[2])
    out[:, : half[1]] = jnp.broadcast_to(jnp.sum(squares[:, :width_q], keepdims=True)[None], half)
    out[:, half[1] :] = jnp.broadcast_to(jnp.sum(squares[:, width_q:], keepdims=True)[None], half)


def final_body(
    sizes, own, other, w0, w1, w2, w3, piece, sums, fq_own, fo_own, wq, wo,
    step_q, step_o, new_q, new_o, copy_q_t, copy_o, held_q, held_o,
):
    core = lax.axis_index("tp") % 2
    y = lax.axis_index("fs") % RING
    rows_q, width_q = wq.shape
    rows = rows_q + wo.shape[0]
    count = own.shape[0]
    for k, ref in enumerate((w0, w1, w2, w3)):
        u = (y + (RING - k)) % RING
        got = ref[...].astype(F32)
        held_q[u // 2, :, u % 2] = got[:, 0:8]
        held_o[0, :, u] = got[:, 8:16]
        held_o[1, :, u] = got[:, 16:24]
    total = jnp.sum(sums[...], axis=0)
    middle = total.shape[0] // 2
    scale_q = 1.0 / jnp.sqrt(total[0:1, :1] / sizes[0] + 0.25)
    scale_o = 1.0 / jnp.sqrt(total[middle : middle + 1, :1] / sizes[1] + 0.25)
    rank = fq_own.shape[1]
    whole = piece[...].reshape(rank, -1)
    for f, w, step, new, scale, direction in (
        (fq_own, wq, step_q, new_q, scale_q, whole[:, :width_q]),
        (fo_own, wo, step_o, new_o, scale_o, whole[:, width_q:]),
    ):
        step_own = contract(f[...], direction, 1, 0) * scale
        step[...] = step_own
        new[...] = w[...] - 0.02 * step_own
    step_all_q = 0.0
    step_all_o = 0.0
    for ref, at in ((own, core), (other, 1 - core)):
        direction = piece[pl.ds(at * (count // 2), count // 2)].reshape(LANES, -1)
        fq = ref[:, :rows_q].reshape(count * rows_q, LANES)
        fo = ref[:, rows_q:rows].reshape(count * (rows - rows_q), LANES)
        step_all_q = step_all_q + contract(fq, direction[:, :width_q], 1, 0)
        step_all_o = step_all_o + contract(fo, direction[:, width_q:], 1, 0)
    q = jnp.concatenate([held_q[0].reshape(-1, LANES), held_q[1].reshape(-1, LANES)[:, : width_q - LANES]], axis=1)
    copy_q_t[...] = (q - 0.02 * (step_all_q * scale_q)).T.astype(BF16)
    o = jnp.concatenate([held_o[0].reshape(-1, LANES), held_o[1].reshape(-1, LANES)], axis=1)
    copy_o[...] = (o - 0.02 * (step_all_o * scale_o)).astype(BF16)


def on_device(
    latent_in,
    query_cot,
    attn_out,
    mix_cot,
    query_weight,
    output_weight,
    query_factor,
    output_factor,
    query_mean,
    query_square,
    output_mean,
    output_square,
):
    count = lax.axis_size("fs")
    columns = lax.axis_size("tp")
    inv_root = 1.0 / math.sqrt(latent_in.shape[0] * count)
    rows_q, width_q = query_weight.shape
    rows_o, width_o = output_weight.shape
    rank = query_factor.shape[1]
    width = width_q + width_o
    rows = rows_q + rows_o
    quarter = 24

    (packed,) = on_chip(
        pack_body,
        [((count, rows + quarter, LANES), BF16)],
        query_factor, output_factor, query_weight, output_weight,
    )
    own = exchange(packed, "fs")
    grad_q_t = contract(query_cot, latent_in, 0, 0).astype(BF16)
    grad_o = contract(attn_out, mix_cot, 0, 0).astype(BF16)
    other = lax.ppermute(own, "tp", [(i, i ^ 1) for i in range(columns)])
    held = [own[:, rows:]]
    for k in range(1, RING):
        pairs = [(i, i // RING * RING + (i + k) % RING) for i in range(count)]
        held.append(lax.ppermute(held[0], "fs", pairs))

    (low,) = on_chip(
        functools.partial(low_body, inv_root, rows_q, rows),
        [((count, rank // count, width), BF16)],
        own, other, grad_q_t, grad_o,
    )
    parts = exchange(low, "fs")
    of_q = (query_mean.shape, F32)
    of_o = (output_mean.shape, F32)
    mean_q, square_q, mean_o, square_o, joined = on_chip(
        moments_body,
        [of_q, of_q, of_o, of_o, ((count, rank // count, width), BF16)],
        parts, query_mean, query_square, output_mean, output_square,
    )
    piece = exchange(joined, "fs")
    (sums,) = on_chip(functools.partial(sums_body, width_q), [((columns, 8, LANES), F32)], piece)
    sums = exchange(sums, "tp")
    sizes = (rank * width_q * columns, rank * width_o * columns)
    step_q, step_o, new_q, new_o, copy_q_t, copy_o = on_chip(
        functools.partial(final_body, sizes),
        [
            ((rows_q, width_q), F32),
            ((rows_o, width_o), F32),
            ((rows_q, width_q), F32),
            ((rows_o, width_o), F32),
            ((width_q, rows_q * count), BF16),
            ((rows_o * count, width_o), BF16),
        ],
        own, other, *held, piece, sums, query_factor, output_factor, query_weight, output_weight,
        scratch=(
            pltpu.VMEM((2, count, 2, 8, LANES), F32),
            pltpu.VMEM((2, count, RING, 8, LANES), F32),
        ),
    )
    return (step_q, step_o, new_q, new_o, copy_q_t.T, copy_o, mean_q, square_q, mean_o, square_o)


def solution(mesh):
    rows = P("fs", None)
    both = P("fs", "tp")
    gathered = P(None, "tp")
    return jax.shard_map(
        on_device,
        mesh=mesh,
        in_specs=(rows, both, rows, both, both, both, rows, rows, both, both, both, both),
        out_specs=(both, both, both, both, gathered, gathered, both, both, both, both),
        check_vma=False,
    )
```

```python
import functools
import math

import jax
import jax.numpy as jnp
from jax import lax
from jax.experimental import pallas as pl
from jax.experimental.pallas import tpu as pltpu
from jax.sharding import PartitionSpec as P

BF16 = jnp.bfloat16
F32 = jnp.float32
LANES = 128
SMALL = 16 * 2**20
RING = 4


def exchange(tiles, axis):
    return lax.all_to_all(tiles, axis, split_axis=0, concat_axis=0, tiled=True)


def contract(left, right, left_dim, right_dim):
    dims = (((left_dim,), (right_dim,)), ((), ()))
    return lax.dot_general(left, right, dims, preferred_element_type=F32)


def near(x):
    return pltpu.with_memory_space_constraint(x, pltpu.VMEM)


def on_chip(body, outs, *args, scratch=(), limit=None, copied=False):
    vmem = pl.BlockSpec(memory_space=pltpu.VMEM)
    return pl.pallas_call(
        body,
        out_shape=tuple(pltpu.VMEM(s, d) if stays else jax.ShapeDtypeStruct(s, d) for s, d, stays in outs),
        in_specs=[vmem] * len(args),
        out_specs=tuple(pl.BlockSpec(memory_space=pl.ANY) if copied else vmem for _ in outs),
        scratch_shapes=list(scratch),
        compiler_params=pltpu.CompilerParams(vmem_limit_bytes=limit),
    )(*args)


def halves(x):
    return x[:, :LANES], x[:, LANES:]


def pack_body(fq, fo, wq, wo, out, tiles, sems):
    count = out.shape[0]
    core = lax.axis_index("tp") % 2
    rows_q, rows_o = fq.shape[0], fo.shape[0]
    rows = rows_q + rows_o
    width_q = wq.shape[1]
    for y in range(RING):
        for f, at in ((fq, 0), (fo, rows_q)):
            left, right = halves(f[...])
            half = jnp.where(core == 0, left.astype(F32), right.astype(F32)).astype(BF16)
            tiles[y, at : at + f.shape[0]] = half
        row, col = y % 2, y // 2
        part = wq[8 * row : 8 * row + 8, col * LANES : min(width_q, (col + 1) * LANES)]
        if part.shape[1] < LANES:
            part = jnp.concatenate([part, jnp.zeros((8, LANES - part.shape[1]), F32)], axis=1)
        left, right = halves(wo[8 * y : 8 * y + 8, :])
        tiles[y, rows:] = jnp.concatenate([part, left, right], axis=0).astype(BF16)
    copies = [
        pltpu.make_async_copy(tiles, out.at[pl.ds(z * RING, RING)], sems.at[z])
        for z in range(count // RING)
    ]
    for copy in copies:
        copy.start()
    for copy in copies:
        copy.wait()


def low_body(inv_root, rows_q, rows, own, other, gq_t, go, out):
    count = own.shape[0]
    core = lax.axis_index("tp") % 2
    width_q = gq_t.shape[0]
    part = (count // 2, LANES * 2 // count, -1)
    for ref, at in ((own, core), (other, 1 - core)):
        fq = ref[:, :rows_q].reshape(count * rows_q, LANES)
        fo = ref[:, rows_q:rows].reshape(count * (rows - rows_q), LANES)
        low_q = contract(gq_t[...], fq, 1, 0).T * inv_root
        low_o = contract(fo, go[...], 0, 0) * inv_root
        to = pl.ds(at * (count // 2), count // 2)
        out[to, :, :width_q] = low_q.reshape(part).astype(BF16)
        out[to, :, width_q:] = low_o.reshape(part).astype(BF16)


def moments_body(parts, mq, sq, mo, so, mq_new, sq_new, mo_new, so_new, out):
    low = jnp.sum(parts[...].astype(F32), axis=0)
    width_q = mq.shape[1]
    count = out.shape[0]
    for piece, mean, square, mean_out, square_out, at in (
        (low[:, :width_q], mq, sq, mq_new, sq_new, slice(0, width_q)),
        (low[:, width_q:], mo, so, mo_new, so_new, slice(width_q, None)),
    ):
        mean_new = 0.8 * mean[...] + 0.2 * piece
        square_new = 0.9 * square[...] + 0.1 * piece * piece
        mean_out[...] = mean_new
        square_out[...] = square_new
        direction = (mean_new / jnp.sqrt(square_new)).astype(BF16)
        out[:, :, at] = jnp.broadcast_to(direction, (count, *direction.shape))


def sums_body(width_q, piece, out):
    x = piece[...].astype(F32)
    squares = jnp.sum(jnp.sum(x * x, axis=0), axis=0, keepdims=True)
    half = (out.shape[0], out.shape[1] // 2, out.shape[2])
    out[:, : half[1]] = jnp.broadcast_to(jnp.sum(squares[:, :width_q], keepdims=True)[None], half)
    out[:, half[1] :] = jnp.broadcast_to(jnp.sum(squares[:, width_q:], keepdims=True)[None], half)


def product_body(own, other, piece, fq_own, fo_own, step_q, step_o, all_q, all_o):
    core = lax.axis_index("tp") % 2
    rows_q, width_q = step_q.shape
    rows = rows_q + step_o.shape[0]
    count = own.shape[0]
    rank = fq_own.shape[1]
    whole = piece[...].reshape(rank, -1)
    step_q[...] = contract(fq_own[...], whole[:, :width_q], 1, 0)
    step_o[...] = contract(fo_own[...], whole[:, width_q:], 1, 0)
    step_all_q = 0.0
    step_all_o = 0.0
    for ref, at in ((own, core), (other, 1 - core)):
        direction = piece[pl.ds(at * (count // 2), count // 2)].reshape(LANES, -1)
        fq = ref[:, :rows_q].reshape(count * rows_q, LANES)
        fo = ref[:, rows_q:rows].reshape(count * (rows - rows_q), LANES)
        step_all_q = step_all_q + contract(fq, direction[:, :width_q], 1, 0)
        step_all_o = step_all_o + contract(fo, direction[:, width_q:], 1, 0)
    all_q[...] = step_all_q.T.astype(BF16)
    all_o[...] = step_all_o.astype(BF16)


def assemble_body(w0, w1, w2, w3, whole_q_t, whole_o, held_q, held_o):
    y = lax.axis_index("fs") % RING
    width_q = whole_q_t.shape[0]
    for k, ref in enumerate((w0, w1, w2, w3)):
        u = (y + (RING - k)) % RING
        got = ref[...].astype(F32)
        held_q[u // 2, :, u % 2] = got[:, 0:8]
        held_o[0, :, u] = got[:, 8:16]
        held_o[1, :, u] = got[:, 16:24]
    for part in range(2):
        at = slice(part * LANES, min(width_q, (part + 1) * LANES))
        whole_q_t[at] = held_q[part].reshape(-1, LANES).T[: at.stop - at.start].astype(BF16)
        at = slice(part * LANES, (part + 1) * LANES)
        whole_o[:, at] = held_o[part].reshape(-1, LANES).astype(BF16)


def final_body(
    sizes, whole_q_t, whole_o, sums, pq_own, po_own, pq_all, po_all, wq, wo,
    step_q, step_o, new_q, new_o, copy_q_t, copy_o,
):
    total = jnp.sum(sums[...], axis=0)
    middle = total.shape[0] // 2
    scale_q = 1.0 / jnp.sqrt(total[0:1, :1] / sizes[0] + 0.25)
    scale_o = 1.0 / jnp.sqrt(total[middle : middle + 1, :1] / sizes[1] + 0.25)
    for p, w, step, new, scale in (
        (pq_own, wq, step_q, new_q, scale_q),
        (po_own, wo, step_o, new_o, scale_o),
    ):
        step_own = p[...] * scale
        step[...] = step_own
        new[...] = w[...] - 0.02 * step_own
    for w, p, copy, scale in ((whole_q_t, pq_all, copy_q_t, scale_q), (whole_o, po_all, copy_o, scale_o)):
        copy[...] = (w[...].astype(F32) - 0.02 * (p[...].astype(F32) * scale)).astype(BF16)


def on_device(
    latent_in,
    query_cot,
    attn_out,
    mix_cot,
    query_weight,
    output_weight,
    query_factor,
    output_factor,
    query_mean,
    query_square,
    output_mean,
    output_square,
):
    count = lax.axis_size("fs")
    columns = lax.axis_size("tp")
    inv_root = 1.0 / math.sqrt(latent_in.shape[0] * count)
    rows_q, width_q = query_weight.shape
    rows_o, width_o = output_weight.shape
    rank = query_factor.shape[1]
    width = width_q + width_o
    rows = rows_q + rows_o
    quarter = 24

    (packed,) = on_chip(
        pack_body,
        [((count, rows + quarter, LANES), BF16, False)],
        query_factor, output_factor, query_weight, output_weight,
        scratch=(
            pltpu.VMEM((RING, rows + quarter, LANES), BF16),
            pltpu.SemaphoreType.DMA((count // RING,)),
        ),
        copied=True,
    )
    own = exchange(packed, "fs")
    grad_q_t = contract(query_cot, latent_in, 0, 0).astype(BF16)
    grad_o = contract(attn_out, mix_cot, 0, 0).astype(BF16)
    other = lax.ppermute(own, "tp", [(i, i ^ 1) for i in range(columns)])
    held = [own[:, rows:]]
    for k in range(1, RING):
        pairs = [(i, i // RING * RING + (i + k) % RING) for i in range(count)]
        held.append(lax.ppermute(held[0], "fs", pairs))

    (low,) = on_chip(
        functools.partial(low_body, inv_root, rows_q, rows),
        [((count, rank // count, width), BF16, True)],
        own, other, near(grad_q_t), near(grad_o),
    )
    parts = exchange(low, "fs")
    of_q = (query_mean.shape, F32, False)
    of_o = (output_mean.shape, F32, False)
    mean_q, square_q, mean_o, square_o, joined = on_chip(
        moments_body,
        [of_q, of_q, of_o, of_o, ((count, rank // count, width), BF16, False)],
        near(parts), query_mean, query_square, output_mean, output_square, limit=SMALL,
    )
    piece = exchange(joined, "fs")
    wholes = on_chip(
        assemble_body,
        [((width_q, rows_q * count), BF16, False), ((rows_o * count, width_o), BF16, False)],
        *held,
        scratch=(
            pltpu.VMEM((2, count, 2, 8, LANES), F32),
            pltpu.VMEM((2, count, RING, 8, LANES), F32),
        ),
    )
    (sums,) = on_chip(
        functools.partial(sums_body, width_q), [((columns, 8, LANES), F32, False)], near(piece), limit=SMALL
    )
    sums = exchange(sums, "tp")
    sizes = (rank * width_q * columns, rank * width_o * columns)
    products = on_chip(
        product_body,
        [
            ((rows_q, width_q), F32, True),
            ((rows_o, width_o), F32, True),
            ((width_q, rows_q * count), BF16, True),
            ((rows_o * count, width_o), BF16, True),
        ],
        own, other, near(piece), query_factor, output_factor,
    )
    step_q, step_o, new_q, new_o, copy_q_t, copy_o = on_chip(
        functools.partial(final_body, sizes),
        [
            ((rows_q, width_q), F32, False),
            ((rows_o, width_o), F32, False),
            ((rows_q, width_q), F32, False),
            ((rows_o, width_o), F32, False),
            ((width_q, rows_q * count), BF16, False),
            ((rows_o * count, width_o), BF16, False),
        ],
        *wholes, near(sums), *map(near, products), query_weight, output_weight,
    )
    return (step_q, step_o, new_q, new_o, copy_q_t.T, copy_o, mean_q, square_q, mean_o, square_o)


def solution(mesh):
    rows = P("fs", None)
    both = P("fs", "tp")
    gathered = P(None, "tp")
    return jax.shard_map(
        on_device,
        mesh=mesh,
        in_specs=(rows, both, rows, both, both, both, rows, rows, both, both, both, both),
        out_specs=(both, both, both, both, gathered, gathered, both, both, both, both),
        check_vma=False,
    )
```

```python
import functools
import math

import jax
import jax.numpy as jnp
from jax import lax
from jax.experimental import pallas as pl
from jax.experimental.pallas import tpu as pltpu
from jax.sharding import PartitionSpec as P

BF16 = jnp.bfloat16
F32 = jnp.float32
LANES = 128
SMALL = 16 * 2**20
FIRST = (6, 2)
RING = 4


def exchange(tiles, axis, order=None):
    groups = None if order is None else [order]
    return lax.all_to_all(
        tiles, axis, split_axis=0, concat_axis=0, tiled=True, axis_index_groups=groups
    )


def contract(left, right, left_dim, right_dim):
    dims = (((left_dim,), (right_dim,)), ((), ()))
    return lax.dot_general(left, right, dims, preferred_element_type=F32)


def near(x):
    return pltpu.with_memory_space_constraint(x, pltpu.VMEM)


FAR, NEAR, BY_HAND = "far", "near", "by hand"


def on_chip(body, outs, *args, scratch=(), limit=None):
    vmem = pl.BlockSpec(memory_space=pltpu.VMEM)
    hand = pl.BlockSpec(memory_space=pl.ANY)
    return pl.pallas_call(
        body,
        out_shape=tuple(pltpu.VMEM(s, d) if at == NEAR else jax.ShapeDtypeStruct(s, d) for s, d, at in outs),
        in_specs=[vmem] * len(args),
        out_specs=tuple(hand if at == BY_HAND else vmem for _, _, at in outs),
        scratch_shapes=list(scratch),
        compiler_params=pltpu.CompilerParams(vmem_limit_bytes=limit),
    )(*args)


def halves(x):
    return x[:, :LANES], x[:, LANES:]


def turned(x, by, axis):
    size = x.shape[axis]
    by %= size
    if by == 0:
        return x
    return jnp.concatenate(
        [lax.slice_in_dim(x, size - by, size, axis=axis), lax.slice_in_dim(x, 0, size - by, axis=axis)], axis=axis
    )


def in_order(x, back=False):
    x = x.reshape(-1, RING, *x.shape[1:])
    for axis, by in enumerate(FIRST):
        x = turned(x, -by if back else by, axis)
    return x.reshape(-1, *x.shape[2:])


def exchange_order(count):
    z, y = FIRST
    return [(i // RING + z) % (count // RING) * RING + (i + y) % RING for i in range(count)]


def pack_body(fq, fo, wq, wo, out, tiles, sems):
    count = out.shape[0]
    core = lax.axis_index("tp") % 2
    rows_q, rows_o = fq.shape[0], fo.shape[0]
    rows = rows_q + rows_o
    width_q = wq.shape[1]
    for y in range(RING):
        for f, at in ((fq, 0), (fo, rows_q)):
            left, right = halves(f[...])
            half = jnp.where(core == 0, left.astype(F32), right.astype(F32)).astype(BF16)
            tiles[y, at : at + f.shape[0]] = half
        to = (y + FIRST[1]) % RING
        row, col = to % 2, to // 2
        part = wq[8 * row : 8 * row + 8, col * LANES : min(width_q, (col + 1) * LANES)]
        if part.shape[1] < LANES:
            part = jnp.concatenate([part, jnp.zeros((8, LANES - part.shape[1]), F32)], axis=1)
        left, right = halves(wo[8 * to : 8 * to + 8, :])
        tiles[y, rows:] = jnp.concatenate([part, left, right], axis=0).astype(BF16)
    copies = [
        pltpu.make_async_copy(tiles, out.at[pl.ds(z * RING, RING)], sems.at[z])
        for z in range(count // RING)
    ]
    for copy in copies:
        copy.start()
    for copy in copies:
        copy.wait()


def low_body(inv_root, rows_q, rows, own, other, gq_t, go, out):
    count = own.shape[0]
    core = lax.axis_index("tp") % 2
    width_q = gq_t.shape[0]
    lows = []
    for ref in (own, other):
        fq = in_order(ref[:, :rows_q]).reshape(count * rows_q, LANES)
        fo = in_order(ref[:, rows_q:rows]).reshape(count * (rows - rows_q), LANES)
        low_q = contract(gq_t[...], fq, 1, 0).T * inv_root
        low_o = contract(fo, go[...], 0, 0) * inv_root
        lows.append((low_q, low_o))
    for mine, others, at in zip(*lows, (slice(0, width_q), slice(width_q, None))):
        low = jnp.concatenate(
            [jnp.where(core == 0, mine, others), jnp.where(core == 0, others, mine)], axis=0
        )
        out[:, :, at] = in_order(low.reshape(count, -1, low.shape[1]), back=True).astype(BF16)


def keep_body(own, other, kept, sems):
    core = lax.axis_index("tp") % 2
    copies = [
        pltpu.make_async_copy(ref, kept.at[at], sems.at[k])
        for k, (ref, at) in enumerate(((own, core), (other, 1 - core)))
    ]
    for copy in copies:
        copy.start()
    for copy in copies:
        copy.wait()


def moments_body(parts, mq, sq, mo, so, mq_new, sq_new, mo_new, so_new, out):
    low = jnp.sum(parts[...].astype(F32), axis=0)
    width_q = mq.shape[1]
    count = out.shape[0]
    for piece, mean, square, mean_out, square_out, at in (
        (low[:, :width_q], mq, sq, mq_new, sq_new, slice(0, width_q)),
        (low[:, width_q:], mo, so, mo_new, so_new, slice(width_q, None)),
    ):
        mean_new = 0.8 * mean[...] + 0.2 * piece
        square_new = 0.9 * square[...] + 0.1 * piece * piece
        mean_out[...] = mean_new
        square_out[...] = square_new
        direction = (mean_new / jnp.sqrt(square_new)).astype(BF16)
        out[:, :, at] = jnp.broadcast_to(direction, (count, *direction.shape))


def sums_body(width_q, piece, out):
    x = piece[...].astype(F32)
    squares = jnp.sum(jnp.sum(x * x, axis=0), axis=0, keepdims=True)
    half = (out.shape[0], out.shape[1] // 2, out.shape[2])
    out[:, : half[1]] = jnp.broadcast_to(jnp.sum(squares[:, :width_q], keepdims=True)[None], half)
    out[:, half[1] :] = jnp.broadcast_to(jnp.sum(squares[:, width_q:], keepdims=True)[None], half)


def product_body(kept, piece, fq_own, fo_own, step_q, step_o, all_q_t, all_o):
    rows_q, width_q = step_q.shape
    rows = rows_q + step_o.shape[0]
    count = kept.shape[1]
    rank = fq_own.shape[1]
    whole = in_order(piece[...]).reshape(rank, -1)
    step_q[...] = contract(fq_own[...], whole[:, :width_q], 1, 0)
    step_o[...] = contract(fo_own[...], whole[:, width_q:], 1, 0)
    step_all_q = 0.0
    step_all_o = 0.0
    for core in range(2):
        direction = whole[core * LANES : (core + 1) * LANES]
        fq = in_order(kept[core, :, :rows_q]).reshape(count * rows_q, LANES)
        fo = in_order(kept[core, :, rows_q:rows]).reshape(count * (rows - rows_q), LANES)
        step_all_q = step_all_q + contract(fq, direction[:, :width_q], 1, 0)
        step_all_o = step_all_o + contract(fo, direction[:, width_q:], 1, 0)
    all_q_t[...] = step_all_q.T.astype(BF16)
    all_o[...] = step_all_o.astype(BF16)


def assemble_body(w0, w1, w2, w3, whole_q_t, whole_o, held_q, held_o):
    y = lax.axis_index("fs") % RING
    width_q = whole_q_t.shape[0]
    for k, ref in enumerate((w0, w1, w2, w3)):
        u = (y + (RING - k)) % RING
        got = in_order(ref[...].astype(F32))
        held_q[u // 2, :, u % 2] = got[:, 0:8]
        held_o[0, :, u] = got[:, 8:16]
        held_o[1, :, u] = got[:, 16:24]
    for part in range(2):
        at = slice(part * LANES, min(width_q, (part + 1) * LANES))
        whole_q_t[at] = held_q[part].reshape(-1, LANES).T[: at.stop - at.start].astype(BF16)
        at = slice(part * LANES, (part + 1) * LANES)
        whole_o[:, at] = held_o[part].reshape(-1, LANES).astype(BF16)


def final_body(
    sizes, whole_q_t, whole_o, sums, pq_own, po_own, pq_all, po_all, wq, wo,
    step_q, step_o, new_q, new_o, copy_q_t, copy_o,
):
    total = jnp.sum(sums[...], axis=0)
    middle = total.shape[0] // 2
    scale_q = 1.0 / jnp.sqrt(total[0:1, :1] / sizes[0] + 0.25)
    scale_o = 1.0 / jnp.sqrt(total[middle : middle + 1, :1] / sizes[1] + 0.25)
    for p, w, step, new, scale in (
        (pq_own, wq, step_q, new_q, scale_q),
        (po_own, wo, step_o, new_o, scale_o),
    ):
        step_own = p[...] * scale
        step[...] = step_own
        new[...] = w[...] - 0.02 * step_own
    for w, p, copy, scale in ((whole_q_t, pq_all, copy_q_t, scale_q), (whole_o, po_all, copy_o, scale_o)):
        copy[...] = (w[...].astype(F32) - 0.02 * (p[...].astype(F32) * scale)).astype(BF16)


def on_device(
    latent_in,
    query_cot,
    attn_out,
    mix_cot,
    query_weight,
    output_weight,
    query_factor,
    output_factor,
    query_mean,
    query_square,
    output_mean,
    output_square,
):
    count = lax.axis_size("fs")
    columns = lax.axis_size("tp")
    inv_root = 1.0 / math.sqrt(latent_in.shape[0] * count)
    rows_q, width_q = query_weight.shape
    rows_o, width_o = output_weight.shape
    rank = query_factor.shape[1]
    width = width_q + width_o
    rows = rows_q + rows_o
    quarter = 24

    (packed,) = on_chip(
        pack_body,
        [((count, rows + quarter, LANES), BF16, BY_HAND)],
        query_factor, output_factor, query_weight, output_weight,
        scratch=(
            pltpu.VMEM((RING, rows + quarter, LANES), BF16),
            pltpu.SemaphoreType.DMA((count // RING,)),
        ),
    )
    own = exchange(packed, "fs", exchange_order(count))
    grad_q_t = contract(query_cot, latent_in, 0, 0).astype(BF16)
    grad_o = contract(attn_out, mix_cot, 0, 0).astype(BF16)
    other = lax.ppermute(own, "tp", [(i, i ^ 1) for i in range(columns)])
    held = [own[:, rows:]]
    for k in range(1, RING):
        pairs = [(i, i // RING * RING + (i + k) % RING) for i in range(count)]
        held.append(lax.ppermute(held[0], "fs", pairs))

    (low,) = on_chip(
        functools.partial(low_body, inv_root, rows_q, rows),
        [((count, rank // count, width), BF16, FAR)],
        near(own), near(other), near(grad_q_t), near(grad_o),
    )
    (kept,) = on_chip(
        keep_body,
        [((2, *own.shape), BF16, BY_HAND)],
        near(own), near(other),
        scratch=(pltpu.SemaphoreType.DMA((2,)),),
    )
    parts = exchange(low, "fs", exchange_order(count))
    of_q = (query_mean.shape, F32, FAR)
    of_o = (output_mean.shape, F32, FAR)
    mean_q, square_q, mean_o, square_o, joined = on_chip(
        moments_body,
        [of_q, of_q, of_o, of_o, ((count, rank // count, width), BF16, FAR)],
        near(parts), query_mean, query_square, output_mean, output_square, limit=SMALL,
    )
    piece = exchange(joined, "fs", exchange_order(count))
    wholes = on_chip(
        assemble_body,
        [((width_q, rows_q * count), BF16, FAR), ((rows_o * count, width_o), BF16, FAR)],
        *held,
        scratch=(
            pltpu.VMEM((2, count, 2, 8, LANES), F32),
            pltpu.VMEM((2, count, RING, 8, LANES), F32),
        ),
    )
    (sums,) = on_chip(
        functools.partial(sums_body, width_q), [((columns, 8, LANES), F32, FAR)], near(piece), limit=SMALL
    )
    sums = exchange(sums, "tp", [i ^ 5 for i in range(columns)])
    sizes = (rank * width_q * columns, rank * width_o * columns)
    products = on_chip(
        product_body,
        [
            ((rows_q, width_q), F32, NEAR),
            ((rows_o, width_o), F32, NEAR),
            ((width_q, rows_q * count), BF16, NEAR),
            ((rows_o * count, width_o), BF16, NEAR),
        ],
        kept, near(piece), query_factor, output_factor,
    )
    step_q, step_o, new_q, new_o, copy_q_t, copy_o = on_chip(
        functools.partial(final_body, sizes),
        [
            ((rows_q, width_q), F32, FAR),
            ((rows_o, width_o), F32, FAR),
            ((rows_q, width_q), F32, FAR),
            ((rows_o, width_o), F32, FAR),
            ((width_q, rows_q * count), BF16, FAR),
            ((rows_o * count, width_o), BF16, FAR),
        ],
        *wholes, near(sums), *map(near, products), query_weight, output_weight,
    )
    return (step_q, step_o, new_q, new_o, copy_q_t.T, copy_o, mean_q, square_q, mean_o, square_o)


def solution(mesh):
    rows = P("fs", None)
    both = P("fs", "tp")
    gathered = P(None, "tp")
    return jax.shard_map(
        on_device,
        mesh=mesh,
        in_specs=(rows, both, rows, both, both, both, rows, rows, both, both, both, both),
        out_specs=(both, both, both, both, gathered, gathered, both, both, both, both),
        check_vma=False,
    )
```

```python
import functools
import math

import jax
import jax.numpy as jnp
from jax import lax
from jax.experimental import pallas as pl
from jax.experimental.pallas import tpu as pltpu
from jax.sharding import PartitionSpec as P

BF16 = jnp.bfloat16
F32 = jnp.float32
LANES = 128
SMALL = 16 * 2**20
FIRST, LOW, DIRECTION = (5, 2), (5, 2), (4, 2)
RING = 4


def exchange(tiles, axis, order=None):
    groups = None if order is None else [order]
    return lax.all_to_all(
        tiles, axis, split_axis=0, concat_axis=0, tiled=True, axis_index_groups=groups
    )


def contract(left, right, left_dim, right_dim):
    dims = (((left_dim,), (right_dim,)), ((), ()))
    return lax.dot_general(left, right, dims, preferred_element_type=F32)


def near(x):
    return pltpu.with_memory_space_constraint(x, pltpu.VMEM)


FAR, NEAR, BY_HAND = "far", "near", "by hand"


def on_chip(body, outs, *args, scratch=(), limit=None):
    vmem = pl.BlockSpec(memory_space=pltpu.VMEM)
    hand = pl.BlockSpec(memory_space=pl.ANY)
    return pl.pallas_call(
        body,
        out_shape=tuple(pltpu.VMEM(s, d) if at == NEAR else jax.ShapeDtypeStruct(s, d) for s, d, at in outs),
        in_specs=[vmem] * len(args),
        out_specs=tuple(hand if at == BY_HAND else vmem for _, _, at in outs),
        scratch_shapes=list(scratch),
        compiler_params=pltpu.CompilerParams(vmem_limit_bytes=limit),
    )(*args)


def halves(x):
    return x[:, :LANES], x[:, LANES:]


def turned(x, by, axis):
    size = x.shape[axis]
    by %= size
    if by == 0:
        return x
    return jnp.concatenate(
        [lax.slice_in_dim(x, size - by, size, axis=axis), lax.slice_in_dim(x, 0, size - by, axis=axis)], axis=axis
    )


def in_order(x, first, back=False):
    x = x.reshape(-1, RING, *x.shape[1:])
    for axis, by in enumerate(first):
        x = turned(x, -by if back else by, axis)
    return x.reshape(-1, *x.shape[2:])


def exchange_order(count, first):
    z, y = first
    return [(i // RING + z) % (count // RING) * RING + (i + y) % RING for i in range(count)]


def folded(q, o):
    return jnp.concatenate([o[..., :4, :], o[..., 4:, :], q[..., :4, :], q[..., 4:, :]], axis=-1)


def unfolded(x, width_q):
    at = x.shape[-1] - 2 * width_q
    o = jnp.concatenate([x[..., : at // 2], x[..., at // 2 : at]], axis=-2)
    q = jnp.concatenate([x[..., at : at + width_q], x[..., at + width_q :]], axis=-2)
    return q, o


def pack_body(fq, fo, wq, wo, out, tiles, sems):
    count = out.shape[0]
    core = lax.axis_index("tp") % 2
    rows_q, rows_o = fq.shape[0], fo.shape[0]
    rows = rows_q + rows_o
    width_q = wq.shape[1]
    for y in range(RING):
        for f, at in ((fq, 0), (fo, rows_q)):
            left, right = halves(f[...])
            half = jnp.where(core == 0, left.astype(F32), right.astype(F32)).astype(BF16)
            tiles[y, at : at + f.shape[0]] = half
        to = (y + FIRST[1]) % RING
        row, col = to % 2, to // 2
        part = wq[8 * row : 8 * row + 8, col * LANES : min(width_q, (col + 1) * LANES)]
        if part.shape[1] < LANES:
            part = jnp.concatenate([part, jnp.zeros((8, LANES - part.shape[1]), F32)], axis=1)
        left, right = halves(wo[8 * to : 8 * to + 8, :])
        tiles[y, rows:] = jnp.concatenate([part, left, right], axis=0).astype(BF16)
    copies = [
        pltpu.make_async_copy(tiles, out.at[pl.ds(z * RING, RING)], sems.at[z])
        for z in range(count // RING)
    ]
    for copy in copies:
        copy.start()
    for copy in copies:
        copy.wait()


def low_body(inv_root, rows_q, rows, own, other, gq_t, go, out):
    count = own.shape[0]
    core = lax.axis_index("tp") % 2
    lows = []
    for ref in (own, other):
        fq = in_order(ref[:, :rows_q], FIRST).reshape(count * rows_q, LANES)
        fo = in_order(ref[:, rows_q:rows], FIRST).reshape(count * (rows - rows_q), LANES)
        low_q = contract(gq_t[...], fq, 1, 0).T * inv_root
        low_o = contract(fo, go[...], 0, 0) * inv_root
        lows.append((low_q, low_o))
    whole = []
    for mine, others in zip(*lows):
        low = jnp.concatenate(
            [jnp.where(core == 0, mine, others), jnp.where(core == 0, others, mine)], axis=0
        )
        whole.append(in_order(low.reshape(count, -1, low.shape[1]), LOW, back=True))
    out[...] = folded(*whole).astype(BF16)


def keep_body(own, other, kept, sems):
    core = lax.axis_index("tp") % 2
    copies = [
        pltpu.make_async_copy(ref, kept.at[at], sems.at[k])
        for k, (ref, at) in enumerate(((own, core), (other, 1 - core)))
    ]
    for copy in copies:
        copy.start()
    for copy in copies:
        copy.wait()


def moments_body(parts, mq, sq, mo, so, mq_new, sq_new, mo_new, so_new, out):
    low_q, low_o = unfolded(jnp.sum(parts[...].astype(F32), axis=0), mq.shape[1])
    directions = []
    for low, mean, square, mean_out, square_out in (
        (low_q, mq, sq, mq_new, sq_new),
        (low_o, mo, so, mo_new, so_new),
    ):
        mean_new = 0.8 * mean[...] + 0.2 * low
        square_new = 0.9 * square[...] + 0.1 * low * low
        mean_out[...] = mean_new
        square_out[...] = square_new
        directions.append(mean_new / jnp.sqrt(square_new))
    out[...] = jnp.broadcast_to(folded(*directions).astype(BF16), out.shape)


def sums_body(width_q, piece, out):
    x = piece[...].astype(F32)
    squares = jnp.sum(jnp.sum(x * x, axis=0), axis=0, keepdims=True)
    at = squares.shape[1] - 2 * width_q
    half = (out.shape[0], out.shape[1] // 2, out.shape[2])
    out[:, : half[1]] = jnp.broadcast_to(jnp.sum(squares[:, at:], keepdims=True)[None], half)
    out[:, half[1] :] = jnp.broadcast_to(jnp.sum(squares[:, :at], keepdims=True)[None], half)


def product_body(kept, piece, fq_own, fo_own, step_q, step_o, all_q_t, all_o):
    rows_q, width_q = step_q.shape
    rows = rows_q + step_o.shape[0]
    count = kept.shape[1]
    rank = fq_own.shape[1]
    direction_q, direction_o = (
        x.reshape(rank, -1).astype(BF16) for x in unfolded(in_order(piece[...].astype(F32), DIRECTION), width_q)
    )
    step_q[...] = contract(fq_own[...], direction_q, 1, 0)
    step_o[...] = contract(fo_own[...], direction_o, 1, 0)
    step_all_q = 0.0
    step_all_o = 0.0
    for core in range(2):
        at = slice(core * LANES, (core + 1) * LANES)
        fq = in_order(kept[core, :, :rows_q], FIRST).reshape(count * rows_q, LANES)
        fo = in_order(kept[core, :, rows_q:rows], FIRST).reshape(count * (rows - rows_q), LANES)
        step_all_q = step_all_q + contract(fq, direction_q[at], 1, 0)
        step_all_o = step_all_o + contract(fo, direction_o[at], 1, 0)
    all_q_t[...] = step_all_q.T.astype(BF16)
    all_o[...] = step_all_o.astype(BF16)


def assemble_body(w0, w1, w2, w3, whole_q_t, whole_o, held_q, held_o):
    y = lax.axis_index("fs") % RING
    width_q = whole_q_t.shape[0]
    for k, ref in enumerate((w0, w1, w2, w3)):
        u = (y + (RING - k)) % RING
        got = in_order(ref[...].astype(F32), FIRST)
        held_q[u // 2, :, u % 2] = got[:, 0:8]
        held_o[0, :, u] = got[:, 8:16]
        held_o[1, :, u] = got[:, 16:24]
    for part in range(2):
        at = slice(part * LANES, min(width_q, (part + 1) * LANES))
        whole_q_t[at] = held_q[part].reshape(-1, LANES).T[: at.stop - at.start].astype(BF16)
        at = slice(part * LANES, (part + 1) * LANES)
        whole_o[:, at] = held_o[part].reshape(-1, LANES).astype(BF16)


def final_body(
    sizes, whole_q_t, whole_o, sums, pq_own, po_own, pq_all, po_all, wq, wo,
    step_q, step_o, new_q, new_o, copy_q_t, copy_o,
):
    total = jnp.sum(sums[...], axis=0)
    middle = total.shape[0] // 2
    scale_q = 1.0 / jnp.sqrt(total[0:1, :1] / sizes[0] + 0.25)
    scale_o = 1.0 / jnp.sqrt(total[middle : middle + 1, :1] / sizes[1] + 0.25)
    for p, w, step, new, scale in (
        (pq_own, wq, step_q, new_q, scale_q),
        (po_own, wo, step_o, new_o, scale_o),
    ):
        step_own = p[...] * scale
        step[...] = step_own
        new[...] = w[...] - 0.02 * step_own
    for w, p, copy, scale in ((whole_q_t, pq_all, copy_q_t, scale_q), (whole_o, po_all, copy_o, scale_o)):
        copy[...] = (w[...].astype(F32) - 0.02 * (p[...].astype(F32) * scale)).astype(BF16)


def on_device(
    latent_in,
    query_cot,
    attn_out,
    mix_cot,
    query_weight,
    output_weight,
    query_factor,
    output_factor,
    query_mean,
    query_square,
    output_mean,
    output_square,
):
    count = lax.axis_size("fs")
    columns = lax.axis_size("tp")
    inv_root = 1.0 / math.sqrt(latent_in.shape[0] * count)
    rows_q, width_q = query_weight.shape
    rows_o, width_o = output_weight.shape
    rank = query_factor.shape[1]
    width = width_q + width_o
    rows = rows_q + rows_o
    quarter = 24

    (packed,) = on_chip(
        pack_body,
        [((count, rows + quarter, LANES), BF16, BY_HAND)],
        query_factor, output_factor, query_weight, output_weight,
        scratch=(
            pltpu.VMEM((RING, rows + quarter, LANES), BF16),
            pltpu.SemaphoreType.DMA((count // RING,)),
        ),
    )
    own = exchange(packed, "fs", exchange_order(count, FIRST))
    grad_q_t = contract(query_cot, latent_in, 0, 0).astype(BF16)
    grad_o = contract(attn_out, mix_cot, 0, 0).astype(BF16)
    other = lax.ppermute(own, "tp", [(i, i ^ 1) for i in range(columns)])
    held = [own[:, rows:]]
    for k in range(1, RING):
        pairs = [(i, i // RING * RING + (i + k) % RING) for i in range(count)]
        held.append(lax.ppermute(held[0], "fs", pairs))

    (low,) = on_chip(
        functools.partial(low_body, inv_root, rows_q, rows),
        [((count, rank // count // 2, 2 * width), BF16, FAR)],
        near(own), near(other), near(grad_q_t), near(grad_o),
    )
    (kept,) = on_chip(
        keep_body,
        [((2, *own.shape), BF16, BY_HAND)],
        near(own), near(other),
        scratch=(pltpu.SemaphoreType.DMA((2,)),),
    )
    parts = exchange(low, "fs", exchange_order(count, LOW))
    of_q = (query_mean.shape, F32, FAR)
    of_o = (output_mean.shape, F32, FAR)
    mean_q, square_q, mean_o, square_o, joined = on_chip(
        moments_body,
        [of_q, of_q, of_o, of_o, ((count, rank // count // 2, 2 * width), BF16, FAR)],
        near(parts), query_mean, query_square, output_mean, output_square, limit=SMALL,
    )
    piece = exchange(joined, "fs", exchange_order(count, DIRECTION))
    wholes = on_chip(
        assemble_body,
        [((width_q, rows_q * count), BF16, FAR), ((rows_o * count, width_o), BF16, FAR)],
        *held,
        scratch=(
            pltpu.VMEM((2, count, 2, 8, LANES), F32),
            pltpu.VMEM((2, count, RING, 8, LANES), F32),
        ),
    )
    (sums,) = on_chip(
        functools.partial(sums_body, width_q), [((columns, 8, LANES), F32, FAR)], near(piece), limit=SMALL
    )
    sums = exchange(sums, "tp", [i ^ 5 for i in range(columns)])
    sizes = (rank * width_q * columns, rank * width_o * columns)
    products = on_chip(
        product_body,
        [
            ((rows_q, width_q), F32, NEAR),
            ((rows_o, width_o), F32, NEAR),
            ((width_q, rows_q * count), BF16, NEAR),
            ((rows_o * count, width_o), BF16, NEAR),
        ],
        kept, near(piece), query_factor, output_factor,
    )
    step_q, step_o, new_q, new_o, copy_q_t, copy_o = on_chip(
        functools.partial(final_body, sizes),
        [
            ((rows_q, width_q), F32, FAR),
            ((rows_o, width_o), F32, FAR),
            ((rows_q, width_q), F32, FAR),
            ((rows_o, width_o), F32, FAR),
            ((width_q, rows_q * count), BF16, FAR),
            ((rows_o * count, width_o), BF16, FAR),
        ],
        *wholes, near(sums), *map(near, products), query_weight, output_weight, limit=24 * 2**20,
    )
    return (step_q, step_o, new_q, new_o, copy_q_t.T, copy_o, mean_q, square_q, mean_o, square_o)


def solution(mesh):
    rows = P("fs", None)
    both = P("fs", "tp")
    gathered = P(None, "tp")
    return jax.shard_map(
        on_device,
        mesh=mesh,
        in_specs=(rows, both, rows, both, both, both, rows, rows, both, both, both, both),
        out_specs=(both, both, both, both, gathered, gathered, both, both, both, both),
        check_vma=False,
    )
```

```python
import functools
import math

import jax
import jax.numpy as jnp
from jax import lax
from jax.experimental import pallas as pl
from jax.experimental.pallas import tpu as pltpu
from jax.sharding import PartitionSpec as P

BF16 = jnp.bfloat16
F32 = jnp.float32
LANES = 128
SMALL = 16 * 2**20
FIRST, LOW, DIRECTION = (5, 2), (5, 2), (4, 2)
RING = 4


def exchange(tiles, axis, order=None):
    groups = None if order is None else [order]
    return lax.all_to_all(
        tiles, axis, split_axis=0, concat_axis=0, tiled=True, axis_index_groups=groups
    )


def contract(left, right, left_dim, right_dim):
    dims = (((left_dim,), (right_dim,)), ((), ()))
    return lax.dot_general(left, right, dims, preferred_element_type=F32)


def near(x):
    return pltpu.with_memory_space_constraint(x, pltpu.VMEM)


FAR, NEAR, BY_HAND = "far", "near", "by hand"


def on_chip(body, outs, *args, scratch=(), limit=None, by_hand=0):
    vmem = pl.BlockSpec(memory_space=pltpu.VMEM)
    hand = pl.BlockSpec(memory_space=pl.ANY)
    return pl.pallas_call(
        body,
        out_shape=tuple(pltpu.VMEM(s, d) if at == NEAR else jax.ShapeDtypeStruct(s, d) for s, d, at in outs),
        in_specs=[hand] * by_hand + [vmem] * (len(args) - by_hand),
        out_specs=tuple(hand if at == BY_HAND else vmem for _, _, at in outs),
        scratch_shapes=list(scratch),
        compiler_params=pltpu.CompilerParams(vmem_limit_bytes=limit),
    )(*args)


def halves(x):
    return x[:, :LANES], x[:, LANES:]


def turned(x, by, axis):
    size = x.shape[axis]
    by %= size
    if by == 0:
        return x
    return jnp.concatenate(
        [lax.slice_in_dim(x, size - by, size, axis=axis), lax.slice_in_dim(x, 0, size - by, axis=axis)], axis=axis
    )


def in_order(x, first, back=False):
    x = x.reshape(-1, RING, *x.shape[1:])
    for axis, by in enumerate(first):
        x = turned(x, -by if back else by, axis)
    return x.reshape(-1, *x.shape[2:])


def exchange_order(count, first):
    z, y = first
    return [(i // RING + z) % (count // RING) * RING + (i + y) % RING for i in range(count)]


def folded(q, o):
    return jnp.concatenate([o[..., :4, :], o[..., 4:, :], q[..., :4, :], q[..., 4:, :]], axis=-1)


def unfolded(x, width_q):
    at = x.shape[-1] - 2 * width_q
    o = jnp.concatenate([x[..., : at // 2], x[..., at // 2 : at]], axis=-2)
    q = jnp.concatenate([x[..., at : at + width_q], x[..., at + width_q :]], axis=-2)
    return q, o


def pack_body(fq, fo, wq, wo, out, tiles, got_q, got_o, reads, sems):
    count = out.shape[0]
    core = lax.axis_index("tp") % 2
    rows_q, rows_o = fq.shape[0], fo.shape[0]
    rows = rows_q + rows_o
    width_q = wq.shape[1]
    weights = [pltpu.make_async_copy(wq, got_q, reads.at[0]), pltpu.make_async_copy(wo, got_o, reads.at[1])]
    columns = pl.ds(pl.multiple_of(core * LANES, LANES), LANES)
    factors = []
    for y in range(RING):
        for k, (f, at) in enumerate(((fq, 0), (fo, rows_q))):
            to = tiles.at[y, at : at + f.shape[0]]
            factors.append(pltpu.make_async_copy(f.at[:, columns], to, reads.at[2 + 2 * y + k]))
    for copy in weights + factors:
        copy.start()
    for copy in weights:
        copy.wait()
    for y in range(RING):
        to = (y + FIRST[1]) % RING
        row, col = to % 2, to // 2
        part = got_q[8 * row : 8 * row + 8, col * LANES : min(width_q, (col + 1) * LANES)]
        if part.shape[1] < LANES:
            part = jnp.concatenate([part, jnp.zeros((8, LANES - part.shape[1]), F32)], axis=1)
        left, right = halves(got_o[8 * to : 8 * to + 8, :])
        tiles[y, rows:] = jnp.concatenate([part, left, right], axis=0).astype(BF16)
    for copy in factors:
        copy.wait()
    copies = [
        pltpu.make_async_copy(tiles, out.at[pl.ds(z * RING, RING)], sems.at[z])
        for z in range(count // RING)
    ]
    for copy in copies:
        copy.start()
    for copy in copies:
        copy.wait()


def low_body(inv_root, rows_q, rows, own, other, gq_t, go, out):
    count = own.shape[0]
    core = lax.axis_index("tp") % 2
    lows = []
    for ref in (own, other):
        fq = in_order(ref[:, :rows_q], FIRST).reshape(count * rows_q, LANES)
        fo = in_order(ref[:, rows_q:rows], FIRST).reshape(count * (rows - rows_q), LANES)
        low_q = contract(gq_t[...], fq, 1, 0).T * inv_root
        low_o = contract(fo, go[...], 0, 0) * inv_root
        lows.append((low_q, low_o))
    whole = []
    for mine, others in zip(*lows):
        low = jnp.concatenate(
            [jnp.where(core == 0, mine, others), jnp.where(core == 0, others, mine)], axis=0
        )
        whole.append(in_order(low.reshape(count, -1, low.shape[1]), LOW, back=True))
    out[...] = folded(*whole).astype(BF16)


def keep_body(own, other, kept, sems):
    core = lax.axis_index("tp") % 2
    copies = [
        pltpu.make_async_copy(ref, kept.at[at], sems.at[k])
        for k, (ref, at) in enumerate(((own, core), (other, 1 - core)))
    ]
    for copy in copies:
        copy.start()
    for copy in copies:
        copy.wait()


def moments_body(parts, mq, sq, mo, so, mq_new, sq_new, mo_new, so_new, out):
    low_q, low_o = unfolded(jnp.sum(parts[...].astype(F32), axis=0), mq.shape[1])
    directions = []
    for low, mean, square, mean_out, square_out in (
        (low_q, mq, sq, mq_new, sq_new),
        (low_o, mo, so, mo_new, so_new),
    ):
        mean_new = 0.8 * mean[...] + 0.2 * low
        square_new = 0.9 * square[...] + 0.1 * low * low
        mean_out[...] = mean_new
        square_out[...] = square_new
        directions.append(mean_new / jnp.sqrt(square_new))
    out[...] = jnp.broadcast_to(folded(*directions).astype(BF16), out.shape)


def sums_body(width_q, piece, out):
    x = piece[...].astype(F32)
    squares = jnp.sum(jnp.sum(x * x, axis=0), axis=0, keepdims=True)
    at = squares.shape[1] - 2 * width_q
    half = (out.shape[0], out.shape[1] // 2, out.shape[2])
    out[:, : half[1]] = jnp.broadcast_to(jnp.sum(squares[:, at:], keepdims=True)[None], half)
    out[:, half[1] :] = jnp.broadcast_to(jnp.sum(squares[:, :at], keepdims=True)[None], half)


def product_body(kept, piece, fq_own, fo_own, step_q, step_o, all_q_t, all_o):
    rows_q, width_q = step_q.shape
    rows = rows_q + step_o.shape[0]
    count = kept.shape[1]
    rank = fq_own.shape[1]
    direction_q, direction_o = (
        x.reshape(rank, -1).astype(BF16) for x in unfolded(in_order(piece[...].astype(F32), DIRECTION), width_q)
    )
    step_q[...] = contract(fq_own[...], direction_q, 1, 0)
    step_o[...] = contract(fo_own[...], direction_o, 1, 0)
    step_all_q = 0.0
    step_all_o = 0.0
    for core in range(2):
        at = slice(core * LANES, (core + 1) * LANES)
        fq = in_order(kept[core, :, :rows_q], FIRST).reshape(count * rows_q, LANES)
        fo = in_order(kept[core, :, rows_q:rows], FIRST).reshape(count * (rows - rows_q), LANES)
        step_all_q = step_all_q + contract(fq, direction_q[at], 1, 0)
        step_all_o = step_all_o + contract(fo, direction_o[at], 1, 0)
    all_q_t[...] = step_all_q.T.astype(BF16)
    all_o[...] = step_all_o.astype(BF16)


def assemble_body(w0, w1, w2, w3, whole_q_t, whole_o, held_q, held_o):
    y = lax.axis_index("fs") % RING
    width_q = whole_q_t.shape[0]
    for k, ref in enumerate((w0, w1, w2, w3)):
        u = (y + (RING - k)) % RING
        got = in_order(ref[...].astype(F32), FIRST)
        held_q[u // 2, :, u % 2] = got[:, 0:8]
        held_o[0, :, u] = got[:, 8:16]
        held_o[1, :, u] = got[:, 16:24]
    for part in range(2):
        at = slice(part * LANES, min(width_q, (part + 1) * LANES))
        whole_q_t[at] = held_q[part].reshape(-1, LANES).T[: at.stop - at.start].astype(BF16)
        at = slice(part * LANES, (part + 1) * LANES)
        whole_o[:, at] = held_o[part].reshape(-1, LANES).astype(BF16)


def final_body(
    sizes, whole_q_t, whole_o, sums, pq_own, po_own, pq_all, po_all, wq, wo,
    step_q, step_o, new_q, new_o, copy_q_t, copy_o,
):
    total = jnp.sum(sums[...], axis=0)
    middle = total.shape[0] // 2
    scale_q = 1.0 / jnp.sqrt(total[0:1, :1] / sizes[0] + 0.25)
    scale_o = 1.0 / jnp.sqrt(total[middle : middle + 1, :1] / sizes[1] + 0.25)
    for p, w, step, new, scale in (
        (pq_own, wq, step_q, new_q, scale_q),
        (po_own, wo, step_o, new_o, scale_o),
    ):
        step_own = p[...] * scale
        step[...] = step_own
        new[...] = w[...] - 0.02 * step_own
    for w, p, copy, scale in ((whole_q_t, pq_all, copy_q_t, scale_q), (whole_o, po_all, copy_o, scale_o)):
        copy[...] = (w[...].astype(F32) - 0.02 * (p[...].astype(F32) * scale)).astype(BF16)


def on_device(
    latent_in,
    query_cot,
    attn_out,
    mix_cot,
    query_weight,
    output_weight,
    query_factor,
    output_factor,
    query_mean,
    query_square,
    output_mean,
    output_square,
):
    count = lax.axis_size("fs")
    columns = lax.axis_size("tp")
    inv_root = 1.0 / math.sqrt(latent_in.shape[0] * count)
    rows_q, width_q = query_weight.shape
    rows_o, width_o = output_weight.shape
    rank = query_factor.shape[1]
    width = width_q + width_o
    rows = rows_q + rows_o
    quarter = 24

    (packed,) = on_chip(
        pack_body,
        [((count, rows + quarter, LANES), BF16, BY_HAND)],
        query_factor, output_factor, query_weight, output_weight,
        scratch=(
            pltpu.VMEM((RING, rows + quarter, LANES), BF16),
            pltpu.VMEM(query_weight.shape, F32),
            pltpu.VMEM(output_weight.shape, F32),
            pltpu.SemaphoreType.DMA((2 + 2 * RING,)),
            pltpu.SemaphoreType.DMA((count // RING,)),
        ),
        by_hand=4,
    )
    own = exchange(packed, "fs", exchange_order(count, FIRST))
    grad_q_t = contract(query_cot, latent_in, 0, 0).astype(BF16)
    grad_o = contract(attn_out, mix_cot, 0, 0).astype(BF16)
    other = lax.ppermute(own, "tp", [(i, i ^ 1) for i in range(columns)])
    held = [own[:, rows:]]
    for k in range(1, RING):
        pairs = [(i, i // RING * RING + (i + k) % RING) for i in range(count)]
        held.append(lax.ppermute(held[0], "fs", pairs))

    (low,) = on_chip(
        functools.partial(low_body, inv_root, rows_q, rows),
        [((count, rank // count // 2, 2 * width), BF16, FAR)],
        near(own), near(other), near(grad_q_t), near(grad_o),
    )
    (kept,) = on_chip(
        keep_body,
        [((2, *own.shape), BF16, BY_HAND)],
        near(own), near(other),
        scratch=(pltpu.SemaphoreType.DMA((2,)),),
    )
    parts = exchange(low, "fs", exchange_order(count, LOW))
    of_q = (query_mean.shape, F32, FAR)
    of_o = (output_mean.shape, F32, FAR)
    mean_q, square_q, mean_o, square_o, joined = on_chip(
        moments_body,
        [of_q, of_q, of_o, of_o, ((count, rank // count // 2, 2 * width), BF16, FAR)],
        near(parts), query_mean, query_square, output_mean, output_square, limit=SMALL,
    )
    piece = exchange(joined, "fs", exchange_order(count, DIRECTION))
    wholes = on_chip(
        assemble_body,
        [((width_q, rows_q * count), BF16, FAR), ((rows_o * count, width_o), BF16, FAR)],
        *held,
        scratch=(
            pltpu.VMEM((2, count, 2, 8, LANES), F32),
            pltpu.VMEM((2, count, RING, 8, LANES), F32),
        ),
    )
    (sums,) = on_chip(
        functools.partial(sums_body, width_q), [((columns, 8, LANES), F32, FAR)], near(piece), limit=SMALL
    )
    sums = exchange(sums, "tp", [i ^ 5 for i in range(columns)])
    sizes = (rank * width_q * columns, rank * width_o * columns)
    products = on_chip(
        product_body,
        [
            ((rows_q, width_q), F32, NEAR),
            ((rows_o, width_o), F32, NEAR),
            ((width_q, rows_q * count), BF16, NEAR),
            ((rows_o * count, width_o), BF16, NEAR),
        ],
        kept, near(piece), query_factor, output_factor,
    )
    step_q, step_o, new_q, new_o, copy_q_t, copy_o = on_chip(
        functools.partial(final_body, sizes),
        [
            ((rows_q, width_q), F32, FAR),
            ((rows_o, width_o), F32, FAR),
            ((rows_q, width_q), F32, FAR),
            ((rows_o, width_o), F32, FAR),
            ((width_q, rows_q * count), BF16, FAR),
            ((rows_o * count, width_o), BF16, FAR),
        ],
        *wholes, near(sums), *map(near, products), query_weight, output_weight, limit=24 * 2**20,
    )
    return (step_q, step_o, new_q, new_o, copy_q_t.T, copy_o, mean_q, square_q, mean_o, square_o)


def solution(mesh):
    rows = P("fs", None)
    both = P("fs", "tp")
    gathered = P(None, "tp")
    return jax.shard_map(
        on_device,
        mesh=mesh,
        in_specs=(rows, both, rows, both, both, both, rows, rows, both, both, both, both),
        out_specs=(both, both, both, both, gathered, gathered, both, both, both, both),
        check_vma=False,
    )
```
